32 devices in a mesh: sp: 4 (over y, x), dp: 8 (over z, core).
Axes of the slice: x: 2, y: 2, z: 4, core: 2. Of those that a mesh axis runs over, the one named last changes fastest.
Arguments:
- tokens: bfloat16 [8, 768, 4096], P('dp', 'sp'), may hold values from -30 to 30
- query_weight: bfloat16 [4096, 512], P('dp', 'sp'), may hold values from -0.09375 to 0.09375
- key_weight: bfloat16 [4096, 512], P('dp', 'sp'), may hold values from -0.09375 to 0.09375
- value_weight: bfloat16 [4096, 512], P('dp', 'sp'), may hold values from -0.09375 to 0.09375
- cum_gate: float32 [8, 4, 768], P('dp', 'sp'), may hold values from -3072 to 0, as said below
Outputs:
- attended: bfloat16 [8, 768, 512], P('dp', 'sp')
The draws below stay inside these ranges and needn't reach their ends.
Inputs may be any that keep to these rules, and one draw needn't show every extreme that they name: `cum_gate`: never rising along positions; the first position holds one step's log gate.
All inputs are finite; a program needn't handle non-finite values.
Results may differ from the reference program's by a relative error of at most 0.0076.
The reference program's roundings to bfloat16 on the way count: a program that leaves them out, or rounds other values in their place, can miss the bound.
Values may be sent and summed in bfloat16 or wider, within the bound.
No kernel may reach another device: no remote copies, remote signals or barrier semaphores. Data moves between devices by JAX's collectives and lax.ppermute only.
A program may use at most 128 MiB of HBM per device.

```python
import jax
import jax.numpy as jnp
from jax import lax

D = 4096
HEAD = 128
TOK_DEV = 192
HEADS = 4
WIDTH = 512
LEN = 768
SEQS = 8


def draw_tokens(key, part):
    base = jnp.clip(jax.random.normal(jax.random.fold_in(key, 11), (SEQS, LEN, D), jnp.float32), -6.0, 6.0)
    return base.astype(jnp.bfloat16)


def shared_matrix(key):
    return jax.random.normal(jax.random.fold_in(key, 21), (D, WIDTH), jnp.float32)


def draw_query_weight(key, part):
    return (jnp.clip(shared_matrix(key), -6.0, 6.0) / 64.0).astype(jnp.bfloat16)


def draw_key_weight(key, part):
    other = jax.random.normal(jax.random.fold_in(key, 22), (D, WIDTH), jnp.float32)
    return (jnp.clip(other, -6.0, 6.0) / 64.0).astype(jnp.bfloat16)


def draw_cum_gate(key, part):
    order = jax.random.permutation(jax.random.fold_in(key, 31), HEADS)
    slow = order < HEADS // 2
    rate = jnp.where(slow, 1.0 / LEN, 1.0 / 40.0)
    blocks = LEN // TOK_DEV
    block_factor = jnp.exp(jax.random.uniform(jax.random.fold_in(key, 32), (SEQS, HEADS, blocks, 1), jnp.float32, -0.69, 0.69))
    block_factor = jnp.broadcast_to(block_factor, (SEQS, HEADS, blocks, TOK_DEV)).reshape(SEQS, HEADS, LEN)
    step_factor = jax.random.uniform(jax.random.fold_in(key, 33), (SEQS, HEADS, LEN), jnp.float32, 0.2, 1.8)
    log_gate = -rate[None, :, None] * block_factor * step_factor
    return jnp.cumsum(log_gate, axis=2).astype(jnp.float32)


def block_scale(own_key, shape, shards, least, top_value):
    gain = 1.0
    for axis_at, shards_of in shards:
        steps = jax.random.uniform(jax.random.fold_in(jax.random.fold_in(own_key, 6), axis_at), (shards_of,), jnp.float32, least / len(shards), top_value / len(shards))
        gain = gain * jnp.repeat(jnp.exp(steps), shape[axis_at] // shards_of).reshape((-1,) + (1,) * (len(shape) - 1 - axis_at))
    return gain


def centred(key, shape, deviation, bound, cuts=(), dtype=jnp.bfloat16):
    values = deviation * jax.random.normal(key, shape, jnp.float32)
    if cuts:
        values = values * block_scale(key, shape, cuts, -0.22, 0.18)
    return jnp.clip(values, -bound, bound).astype(dtype)


def setup_inputs(seed: int = 0) -> dict:
    seeds = jax.random.split(jax.random.key(seed), 6)
    tokens = draw_tokens(jax.random.fold_in(seeds[5], 71), 0)
    query_weight = draw_query_weight(jax.random.fold_in(seeds[5], 71), 0)
    key_weight = draw_key_weight(jax.random.fold_in(seeds[5], 71), 0)
    value_weight = centred(seeds[3], (D, WIDTH), D ** -0.5, 0.09375, ((0, 8), (1, 4)))
    cum_gate = draw_cum_gate(jax.random.fold_in(seeds[5], 71), 0)
    return {"tokens": tokens, "query_weight": query_weight, "key_weight": key_weight, "value_weight": value_weight, "cum_gate": cum_gate}


block_rows = 512


def attend(queries, keys, values, gates):
    length = queries.shape[0]
    scale = queries.shape[1] ** -0.5
    pieces = []
    for start in range(0, length, block_rows):
        finish = min(start + block_rows, length)
        scores = jnp.dot(queries[start:finish], keys[:finish].T, preferred_element_type=jnp.float32) * scale
        scores = scores + gates[start:finish, None] - gates[None, :finish]
        rows_at = start + lax.broadcasted_iota(jnp.int32, scores.shape, 0)
        cols_at = lax.broadcasted_iota(jnp.int32, scores.shape, 1)
        scores = jnp.where(cols_at <= rows_at, scores, -1e30)
        top = jnp.max(scores, axis=1, keepdims=True)
        weights = jnp.exp(scores - top)
        total = jnp.sum(weights, axis=1, keepdims=True)
        summed = jnp.dot(weights.astype(jnp.bfloat16), values[:finish], preferred_element_type=jnp.float32)
        pieces.append((summed / total).astype(jnp.bfloat16))
    return jnp.concatenate(pieces, axis=0)


def reference(tokens, query_weight, key_weight, value_weight, cum_gate):
    def one_sequence(inputs):
        rows, gates = inputs
        queries = jnp.dot(rows, query_weight, preferred_element_type=jnp.float32).astype(jnp.bfloat16)
        keys = jnp.dot(rows, key_weight, preferred_element_type=jnp.float32).astype(jnp.bfloat16)
        values = jnp.dot(rows, value_weight, preferred_element_type=jnp.float32).astype(jnp.bfloat16)

        def by_head(array):
            return jnp.transpose(array.reshape(LEN, HEADS, HEAD), (1, 0, 2))

        heads_out = lax.map(lambda group: attend(group[0], group[1], group[2], group[3]),
                            (by_head(queries), by_head(keys), by_head(values), gates))
        return jnp.transpose(heads_out, (1, 0, 2)).reshape(LEN, HEADS * HEAD)

    return lax.map(one_sequence, (tokens, cum_gate))
```

```python
import math

import jax
import jax.numpy as jnp
from jax import lax
from jax.sharding import PartitionSpec as P


block_rows = 512


def attend(queries, keys, values, gates):
    length = queries.shape[0]
    scale = queries.shape[1] ** (-0.5)
    pieces = []
    for start in range(0, length, block_rows):
        finish = min(start + block_rows, length)
        scores = (
            jnp.dot(queries[start:finish], keys[:finish].T, preferred_element_type=jnp.float32)
            * scale
        )
        scores = scores + gates[start:finish, None] - gates[None, :finish]
        rows_at = start + lax.broadcasted_iota(jnp.int32, scores.shape, 0)
        cols_at = lax.broadcasted_iota(jnp.int32, scores.shape, 1)
        scores = jnp.where(cols_at <= rows_at, scores, -1e30)
        top = jnp.max(scores, axis=1, keepdims=True)
        weights = jnp.exp(scores - top)
        total = jnp.sum(weights, axis=1, keepdims=True)
        summed = jnp.dot(
            weights.astype(jnp.bfloat16), values[:finish], preferred_element_type=jnp.float32
        )
        pieces.append((summed / total).astype(jnp.bfloat16))
    return jnp.concatenate(pieces, axis=0)


def make_body(sp, dp):
    cores = 2
    planes = dp // cores
    side = math.isqrt(sp)

    def send(array, axis, count, target):
        return lax.ppermute(array, axis, [(i, target(i)) for i in range(count)])

    def shift_x(k):
        return lambda i: i // side * side + (i + k) % side

    def shift_y(k):
        return lambda i: (i // side + k) % side * side + i % side

    def shift_z(k):
        return lambda i: (i + k * cores) % dp

    def body(tokens, query_weight, key_weight, value_weight, cum_gate):
        width = query_weight.shape[1]
        own = tokens[0]
        rows = own.shape[0]
        half = rows // 2
        s = lax.axis_index("sp")
        d = lax.axis_index("dp")
        y, x = s // side, s % side
        z, core = d // cores, d % cores
        local = jnp.concatenate([query_weight, key_weight, value_weight], axis=1)
        first, second = own[:half], own[half:]

        chunks = {(0, 0): [first, second]}
        for k in range(1, side):
            late = send(second, "sp", sp, shift_x(k))
            chunks[(0, k)] = [send(first, "sp", sp, shift_x(k)), late]
            chunks[(k, 0)] = [send(first, "sp", sp, shift_y(k)), send(second, "sp", sp, shift_y(k))]
        stripes = [local]
        for k in range(1, planes):
            stripes.append(send(local, "dp", dp, shift_z(k)))
        for j in range(1, side):
            for k in range(1, side):
                early = send(chunks[(j, 0)][0], "sp", sp, shift_x(k))
                late = send(chunks[(0, k)][1], "sp", sp, shift_y(j))
                chunks[(j, k)] = [early, late]
        whole = jnp.zeros((planes, cores) + local.shape, local.dtype)
        for k in range(planes):
            stripe = stripes[k]
            twin = send(stripe, "dp", dp, lambda i: i // cores * cores + (i + 1) % cores)
            at = (z - k) % planes
            whole = lax.dynamic_update_slice(whole, stripe[None, None], (at, core, 0, 0))
            whole = lax.dynamic_update_slice(whole, twin[None, None], (at, (core + 1) % cores, 0, 0))
        stacked = whole.reshape(dp * local.shape[0], local.shape[1])

        projected = jnp.zeros((side, side, rows, 3 * width), jnp.bfloat16)
        for (j, k), parts in chunks.items():
            for n, part in enumerate(parts):
                piece = jnp.dot(part, stacked, preferred_element_type=jnp.float32)
                piece = piece.astype(jnp.bfloat16)
                at = ((y - j) % side, (x - k) % side, n * half, 0)
                projected = lax.dynamic_update_slice(projected, piece[None, None], at)
        projected = projected.reshape(sp * rows, 3 * width)
        queries = projected[:, :width]
        keys = projected[:, width : 2 * width]
        values = projected[:, 2 * width :]
        head_out = attend(queries, keys, values, cum_gate[0, 0])
        gathered = lax.all_to_all(head_out, "sp", split_axis=0, concat_axis=1, tiled=True)
        return gathered[None]

    return body


def solution(mesh):
    in_specs = (
        P("dp", "sp", None),
        P("dp", "sp"),
        P("dp", "sp"),
        P("dp", "sp"),
        P("dp", "sp", None),
    )
    out_specs = P("dp", "sp", None)
    body = make_body(mesh.shape["sp"], mesh.shape["dp"])

    return jax.shard_map(body, mesh=mesh, in_specs=in_specs, out_specs=out_specs, check_vma=False)
```

```python
import math

import jax
import jax.numpy as jnp
from jax import lax
from jax.sharding import PartitionSpec as P


block_rows = 1024


def attend(queries, keys, values, gates, places):
    length = queries.shape[0]
    scale = queries.shape[1] ** (-0.5)
    pieces = []
    for start in range(0, length, block_rows):
        finish = min(start + block_rows, length)
        scores = (
            jnp.dot(queries[start:finish], keys.T, preferred_element_type=jnp.float32) * scale
        )
        scores = scores + gates[start:finish, None] - gates[None, :]
        scores = jnp.where(places[None, :] <= places[start:finish, None], scores, -1e30)
        top = jnp.max(scores, axis=1, keepdims=True)
        weights = jnp.exp(scores - top)
        total = jnp.sum(weights, axis=1, keepdims=True)
        summed = jnp.dot(
            weights.astype(jnp.bfloat16), values, preferred_element_type=jnp.float32
        )
        pieces.append((summed / total).astype(jnp.bfloat16))
    return jnp.concatenate(pieces, axis=0)


def make_body(sp, dp):
    cores = 2
    planes = dp // cores
    side = math.isqrt(sp)

    def send(array, axis, count, target):
        return lax.ppermute(array, axis, [(i, target(i)) for i in range(count)])

    def shift(j, k):
        return lambda i: (i // side + j) % side * side + (i % side + k) % side

    def shift_z(k):
        return lambda i: (i + k * cores) % dp

    def twin_of(i):
        return i // cores * cores + (i + 1) % cores

    def body(tokens, query_weight, key_weight, value_weight, cum_gate):
        width = query_weight.shape[1]
        own = tokens[0]
        rows = own.shape[0]
        half, quarter = rows // 2, rows // 4
        s = lax.axis_index("sp")
        d = lax.axis_index("dp")
        y, x = s // side, s % side
        z, core = d // cores, d % cores
        local = jnp.concatenate([query_weight, key_weight, value_weight], axis=1)
        lower = [own[:quarter], own[quarter:half]]
        upper = [own[half : half + quarter], own[half + quarter :]]

        chunks = {(0, 0): [own]}
        early_y, early_x = {}, {}
        for k in range(1, side):
            early_x[k] = [send(part, "sp", sp, shift(0, k)) for part in upper]
            early_y[k] = [send(part, "sp", sp, shift(k, 0)) for part in lower]
            late_x = send(own[:half], "sp", sp, shift(0, k))
            late_y = send(own[half:], "sp", sp, shift(k, 0))
            chunks[(0, k)] = [late_x] + early_x[k]
            chunks[(k, 0)] = early_y[k] + [late_y]
        stripes = [local]
        for k in range(1, planes):
            stripes.append(send(local, "dp", dp, shift_z(k)))
        for j in range(1, side):
            for k in range(1, side):
                chunks[(j, k)] = [send(part, "sp", sp, shift(0, k)) for part in early_y[j]] + [
                    send(part, "sp", sp, shift(j, 0)) for part in early_x[k]
                ]
        whole = jnp.zeros((planes, cores) + local.shape, local.dtype)
        for k in range(planes):
            stripe = stripes[k]
            twin = send(stripe, "dp", dp, twin_of)
            at = (z - k) % planes
            whole = lax.dynamic_update_slice(whole, stripe[None, None], (at, core, 0, 0))
            whole = lax.dynamic_update_slice(whole, twin[None, None], (at, (core + 1) % cores, 0, 0))
        stacked = whole.reshape(dp * local.shape[0], local.shape[1])

        projected, gates, places = [], [], []
        for (j, k), parts in chunks.items():
            for part in parts:
                piece = jnp.dot(part, stacked, preferred_element_type=jnp.float32)
                projected.append(piece.astype(jnp.bfloat16))
            start = ((y - j) % side * side + (x - k) % side) * rows
            gates.append(lax.dynamic_slice(cum_gate[0, 0], (start,), (rows,)))
            places.append(start + lax.iota(jnp.int32, rows))
        projected = jnp.concatenate(projected, axis=0)
        queries = projected[:, :width]
        keys = projected[:, width : 2 * width]
        values = projected[:, 2 * width :]
        head_out = attend(queries, keys, values, jnp.concatenate(gates), jnp.concatenate(places))
        gathered = jnp.zeros((rows, sp * width), head_out.dtype)
        order = list(enumerate(chunks))
        for n, (j, k) in sorted(order, key=lambda entry: -sum(entry[1])):
            part = head_out[n * rows : (n + 1) * rows]
            if (j, k) != (0, 0):
                part = send(part, "sp", sp, shift(-j, -k))
            head = (y + j) % side * side + (x + k) % side
            gathered = lax.dynamic_update_slice(gathered, part, (0, head * width))
        return gathered[None]

    return body


def solution(mesh):
    in_specs = (
        P("dp", "sp", None),
        P("dp", "sp"),
        P("dp", "sp"),
        P("dp", "sp"),
        P("dp", "sp", None),
    )
    out_specs = P("dp", "sp", None)
    body = make_body(mesh.shape["sp"], mesh.shape["dp"])

    return jax.shard_map(body, mesh=mesh, in_specs=in_specs, out_specs=out_specs, check_vma=False)
```

```python
import math

import jax
import jax.numpy as jnp
from jax import lax
from jax.sharding import PartitionSpec as P


block_rows = 1024


def attend(queries, keys, values, gates, places):
    length = queries.shape[0]
    scale = queries.shape[1] ** (-0.5)
    pieces = []
    for start in range(0, length, block_rows):
        finish = min(start + block_rows, length)
        scores = (
            jnp.dot(queries[start:finish], keys.T, preferred_element_type=jnp.float32) * scale
        )
        scores = scores + gates[start:finish, None] - gates[None, :]
        scores = jnp.where(places[None, :] <= places[start:finish, None], scores, -1e30)
        top = jnp.max(scores, axis=1, keepdims=True)
        weights = jnp.exp(scores - top)
        total = jnp.sum(weights, axis=1, keepdims=True)
        summed = jnp.dot(
            weights.astype(jnp.bfloat16), values, preferred_element_type=jnp.float32
        )
        pieces.append((summed / total).astype(jnp.bfloat16))
    return jnp.concatenate(pieces, axis=0)


def make_body(sp, dp):
    cores = 2
    planes = dp // cores
    side = math.isqrt(sp)

    def send(array, axis, count, target):
        return lax.ppermute(array, axis, [(i, target(i)) for i in range(count)])

    def shift(j, k):
        return lambda i: (i // side + j) % side * side + (i % side + k) % side

    def shift_z(k):
        return lambda i: (i + k * cores) % dp

    def twin_of(i):
        return i // cores * cores + (i + 1) % cores

    def body(tokens, query_weight, key_weight, value_weight, cum_gate):
        width = query_weight.shape[1]
        own = tokens[0]
        rows = own.shape[0]
        half = rows // 2
        s = lax.axis_index("sp")
        d = lax.axis_index("dp")
        y, x = s // side, s % side
        z, core = d // cores, d % cores
        local = jnp.concatenate([query_weight, key_weight, value_weight], axis=1)

        chunks = {(0, 0): own}
        lower = {}
        for k in range(1, side):
            chunks[(0, k)] = send(own, "sp", sp, shift(0, k))
            lower[k] = send(own[:half], "sp", sp, shift(k, 0))
            upper = send(own[half:], "sp", sp, shift(k, 0))
            chunks[(k, 0)] = jnp.concatenate([lower[k], upper], axis=0)
        stripes = [local]
        for k in range(1, planes):
            stripes.append(send(local, "dp", dp, shift_z(k)))
        for j in range(1, side):
            for k in range(1, side):
                first = send(lower[j], "sp", sp, shift(0, k))
                second = send(chunks[(0, k)][half:], "sp", sp, shift(j, 0))
                chunks[(j, k)] = jnp.concatenate([first, second], axis=0)
        whole = jnp.zeros((planes, cores) + local.shape, local.dtype)
        for k in range(planes):
            stripe = stripes[k]
            twin = send(stripe, "dp", dp, twin_of)
            at = (z - k) % planes
            whole = lax.dynamic_update_slice(whole, stripe[None, None], (at, core, 0, 0))
            whole = lax.dynamic_update_slice(whole, twin[None, None], (at, (core + 1) % cores, 0, 0))
        stacked = whole.reshape(dp * local.shape[0], local.shape[1])

        projected, gates, places = [], [], []
        for (j, k), part in chunks.items():
            piece = jnp.dot(part, stacked, preferred_element_type=jnp.float32)
            projected.append(piece.astype(jnp.bfloat16))
            start = ((y - j) % side * side + (x - k) % side) * rows
            gates.append(lax.dynamic_slice(cum_gate[0, 0], (start,), (rows,)))
            places.append(start + lax.iota(jnp.int32, rows))
        projected = jnp.concatenate(projected, axis=0)
        queries = projected[:, :width]
        keys = projected[:, width : 2 * width]
        values = projected[:, 2 * width :]
        head_out = attend(queries, keys, values, jnp.concatenate(gates), jnp.concatenate(places))
        gathered = jnp.zeros((rows, sp * width), head_out.dtype)
        order = list(enumerate(chunks))
        for n, (j, k) in sorted(order, key=lambda entry: -sum(entry[1])):
            part = head_out[n * rows : (n + 1) * rows]
            if (j, k) != (0, 0):
                part = send(part, "sp", sp, shift(-j, -k))
            head = (y + j) % side * side + (x + k) % side
            gathered = lax.dynamic_update_slice(gathered, part, (0, head * width))
        return gathered[None]

    return body


def solution(mesh):
    in_specs = (
        P("dp", "sp", None),
        P("dp", "sp"),
        P("dp", "sp"),
        P("dp", "sp"),
        P("dp", "sp", None),
    )
    out_specs = P("dp", "sp", None)
    body = make_body(mesh.shape["sp"], mesh.shape["dp"])

    return jax.shard_map(body, mesh=mesh, in_specs=in_specs, out_specs=out_specs, check_vma=False)
```

```python
import math

import jax
import jax.numpy as jnp
from jax import lax
from jax.sharding import PartitionSpec as P


block_rows = 1024


def attend(queries, keys, values, gates, places):
    length = queries.shape[0]
    scale = queries.shape[1] ** (-0.5)
    pieces = []
    for start in range(0, length, block_rows):
        finish = min(start + block_rows, length)
        scores = (
            jnp.dot(queries[start:finish], keys.T, preferred_element_type=jnp.float32) * scale
        )
        scores = scores + gates[start:finish, None] - gates[None, :]
        scores = jnp.where(places[None, :] <= places[start:finish, None], scores, -1e30)
        top = jnp.max(scores, axis=1, keepdims=True)
        weights = jnp.exp(scores - top)
        total = jnp.sum(weights, axis=1, keepdims=True)
        summed = jnp.dot(
            weights.astype(jnp.bfloat16), values, preferred_element_type=jnp.float32
        )
        pieces.append((summed / total).astype(jnp.bfloat16))
    return jnp.concatenate(pieces, axis=0)


def make_body(sp, dp):
    cores = 2
    planes = dp // cores
    side = math.isqrt(sp)

    def send(array, axis, count, target):
        return lax.ppermute(array, axis, [(i, target(i)) for i in range(count)])

    def shift(j, k):
        return lambda i: (i // side + j) % side * side + (i % side + k) % side

    def shift_z(k):
        return lambda i: (i + k * cores) % dp

    def twin_of(i):
        return i // cores * cores + (i + 1) % cores

    def body(tokens, query_weight, key_weight, value_weight, cum_gate):
        width = query_weight.shape[1]
        own = tokens[0]
        rows = own.shape[0]
        cut = rows // 2 + rows // 12
        s = lax.axis_index("sp")
        d = lax.axis_index("dp")
        y, x = s // side, s % side
        z, core = d // cores, d % cores
        local = jnp.concatenate([query_weight, key_weight, value_weight], axis=1)

        chunks = {(0, 0): own}
        lower = {}
        for k in range(1, side):
            chunks[(0, k)] = send(own, "sp", sp, shift(0, k))
            lower[k] = send(own[:cut], "sp", sp, shift(k, 0))
            upper = send(own[cut:], "sp", sp, shift(k, 0))
            chunks[(k, 0)] = jnp.concatenate([lower[k], upper], axis=0)
        stripes = [local]
        for k in range(1, planes):
            stripes.append(send(local, "dp", dp, shift_z(k)))
        for j in range(1, side):
            for k in range(1, side):
                first = send(lower[j], "sp", sp, shift(0, k))
                second = send(chunks[(0, k)][cut:], "sp", sp, shift(j, 0))
                chunks[(j, k)] = jnp.concatenate([first, second], axis=0)
        whole = jnp.zeros((planes, cores) + local.shape, local.dtype)
        for k in range(planes):
            stripe = stripes[k]
            twin = send(stripe, "dp", dp, twin_of)
            at = (z - k) % planes
            whole = lax.dynamic_update_slice(whole, stripe[None, None], (at, core, 0, 0))
            whole = lax.dynamic_update_slice(whole, twin[None, None], (at, (core + 1) % cores, 0, 0))
        stacked = whole.reshape(dp * local.shape[0], local.shape[1])

        projected, gates, places = [], [], []
        for (j, k), part in chunks.items():
            piece = jnp.dot(part, stacked, preferred_element_type=jnp.float32)
            projected.append(piece.astype(jnp.bfloat16))
            start = ((y - j) % side * side + (x - k) % side) * rows
            gates.append(lax.dynamic_slice(cum_gate[0, 0], (start,), (rows,)))
            places.append(start + lax.iota(jnp.int32, rows))
        projected = jnp.concatenate(projected, axis=0)
        queries = projected[:, :width]
        keys = projected[:, width : 2 * width]
        values = projected[:, 2 * width :]
        head_out = attend(queries, keys, values, jnp.concatenate(gates), jnp.concatenate(places))
        received = {}
        for n, (j, k) in sorted(enumerate(chunks), key=lambda entry: -sum(entry[1])):
            part = head_out[n * rows : (n + 1) * rows]
            received[j, k] = part if (j, k) == (0, 0) else send(part, "sp", sp, shift(-j, -k))
        gathered = jnp.zeros((rows, sp * width), head_out.dtype)
        for (j, k), part in received.items():
            if (j, k) == (0, 0):
                gathered = lax.dynamic_update_slice(gathered, part, (0, s * width))
        for (j, k), part in received.items():
            if (j, k) != (0, 0):
                head = (y + j) % side * side + (x + k) % side
                gathered = lax.dynamic_update_slice(gathered, part, (0, head * width))
        return gathered[None]

    return body


def solution(mesh):
    in_specs = (
        P("dp", "sp", None),
        P("dp", "sp"),
        P("dp", "sp"),
        P("dp", "sp"),
        P("dp", "sp", None),
    )
    out_specs = P("dp", "sp", None)
    body = make_body(mesh.shape["sp"], mesh.shape["dp"])

    return jax.shard_map(body, mesh=mesh, in_specs=in_specs, out_specs=out_specs, check_vma=False)
```
